32 devices in a mesh: fs: 8 (over z, x), tp: 4 (over y, core).
Axes of the slice: x: 2, y: 2, z: 4, core: 2. Of those that a mesh axis runs over, the one named last changes fastest.
Arguments:
- tokens: bfloat16 [1024, 2048], P('fs', 'tp'), may hold values from -6 to 6
- routes: int32 [1024, 2], P('fs'), may hold values from 0 to 3, all different within a row; in each aligned block of 128 rows (0 to 127, 128 to 255, ...) at most 96 rows name the same one
- route_weight: float32 [1024, 2], P('fs'), may hold values from 0.1 to 1
- norm_gain: float32 [2048], P('fs'), may hold values from 0.1 to 1.9
- expert_gate: float32 [4, 2048, 512], P(None, 'fs', 'tp'), may hold values from -0.125 to 0.125
- expert_up: float32 [4, 2048, 512], P(None, 'fs', 'tp'), may hold values from -0.125 to 0.125
- expert_down: float32 [4, 2048, 512], P(None, 'fs', 'tp'), may hold values from -0.25 to 0.25
- shared_gate: float32 [2048, 512], P('fs', 'tp'), may hold values from -0.125 to 0.125
- shared_up: float32 [2048, 512], P('fs', 'tp'), may hold values from -0.125 to 0.125
- shared_down: float32 [512, 2048], P('tp', 'fs'), may hold values from -0.25 to 0.25
Outputs:
- mixed: bfloat16 [1024, 2048], P('fs', 'tp')
- gate_sampler: bfloat16 [8, 2048, 256], P('fs', None, 'tp')
- up_sampler: bfloat16 [8, 2048, 256], P('fs', None, 'tp')
- down_sampler: bfloat16 [8, 2048, 256], P('fs', 'tp')
- shared_gate_out: bfloat16 [2048, 512], P(None, 'tp')
- shared_up_out: bfloat16 [2048, 512], P(None, 'tp')
- shared_down_out: bfloat16 [512, 2048], P('tp')
The draws below stay inside these ranges and needn't reach their ends.
Inputs may be any that keep to these rules, and one draw needn't show every extreme that they name: `routes`: each row names 2 different experts. In each aligned block of 128 rows no expert is named by more than 96 rows, a bound that some block reaches.
All inputs are finite; a program needn't handle non-finite values.
Results may differ from the reference program's by a relative error of at most 0.009.
Values may be sent and summed in bfloat16 or wider, within the bound.
No kernel may reach another device: no remote copies, remote signals or barrier semaphores. Data moves between devices by JAX's collectives and lax.ppermute only.
A program may use at most 64 MiB of HBM per device.

```python
import math
import jax
import jax.numpy as jnp
import numpy as np
from jax import lax

D = 2048
FF = 512
TOP_K = 2
TOK_DEV = 128
EXPERTS = 4
UNITS = 64
SHARED_BLOCK = 128
CAP = 96
TOKENS = 1024
N_FS = 8
N_TP = 4


def steps_of(rng, shape, split, least, high):
    gain = 1.0
    for dim, blocks in split:
        heights = jax.random.uniform(jax.random.fold_in(jax.random.fold_in(rng, 6), dim), (blocks,), jnp.float32, least / len(split), high / len(split))
        gain = gain * jnp.repeat(jnp.exp(heights), shape[dim] // blocks).reshape((-1,) + (1,) * (len(shape) - 1 - dim))
    return gain


def routed_block(own_key, own, number, rows, number_of, top, most, slope):
    sequence = jax.random.permutation(own_key, number_of)
    heavy_load, ordinary = shares(number_of, rows * top, most, slope, True), shares(number_of, rows * top, most, slope, False)
    places = jnp.arange(number_of)

    def named(sizes, turn):
        used = int((sizes > 0).sum())
        fixed = max(1, used // 4)
        passed = fixed + (places - fixed + turn * (used - fixed)) % max(1, number_of - fixed)
        return jnp.zeros((number_of,), jnp.int32).at[sequence[jnp.where(places < fixed, places, passed)]].set(jnp.asarray(sizes, jnp.int32))

    sizes = jnp.where(number % 4 == 0, named(heavy_load, number // 4), named(ordinary, number - number // 4 - 1))
    mixed = jax.random.permutation(jax.random.fold_in(own, 3), number_of)
    giver, sink = mixed[0:number_of // 2 * 2:2], mixed[1:number_of // 2 * 2:2]
    margin = jnp.minimum(sizes[giver] - 1, most - sizes[sink]) // 2
    margin = jnp.where((giver == sequence[0]) | (sink == sequence[0]) | (sizes[sink] == 0), 0, jnp.maximum(margin, 0))
    passed = jax.random.randint(jax.random.fold_in(own, 4), (number_of // 2,), 0, 1 << 20) % (margin + 1)
    sizes = sizes.at[giver].add(-passed).at[sink].add(passed)
    items = jnp.searchsorted(jnp.cumsum(sizes), jnp.arange(rows * top), side="right").astype(jnp.int32)
    table = items.reshape(top, rows).T
    table = table[jax.random.permutation(jax.random.fold_in(own, 1), rows)]
    turn = jax.random.randint(jax.random.fold_in(own, 2), (rows, 1), 0, top)
    return jnp.take_along_axis(table, (jnp.arange(top)[None, :] + turn) % top, axis=1)


def shares(amount, total, limit, lean, full):
    portions = [(1 << 20) // math.isqrt(rank ** lean) + 1 for rank in range(1, amount + 1)]
    largest = limit if full else min(limit, max(-(-total // amount), total * portions[0] // sum(portions)))
    least = 1 if total - largest >= amount - 1 else 0
    given, rest = [largest] + [least] * (amount - 1), total - largest - least * (amount - 1)
    while rest > 0:
        movable = [i for i in range(1, amount) if given[i] < largest] or [i for i in range(1, amount) if given[i] < limit]
        mass, budget = sum([portions[i] for i in movable]), rest
        for i in movable:
            addition = min(limit - given[i], max(1, budget * portions[i] // mass), rest)
            given[i] = given[i] + addition
            rest = rest - addition
    return np.array(given)


def noise(stream_key, extent, width, bound, pieces=(), held_as=jnp.bfloat16):
    gain = steps_of(stream_key, extent, pieces, -0.22, 0.18) if pieces else 1.0
    values = jax.random.normal(stream_key, extent, jnp.float32) * width * gain
    return jnp.minimum(jnp.maximum(values, -bound), bound).astype(held_as)


def setup_inputs(seed: int = 0) -> dict:
    keys = jax.random.split(jax.random.key(seed), 11)
    tokens = noise(keys[0], (TOKENS, D), 1.0, 6.0, ((0, 8), (1, 4)))
    routes_keys = jax.random.split(jax.random.fold_in(keys[1], 1), TOKENS // TOK_DEV)
    routes_turns = jax.random.permutation(jax.random.fold_in(keys[1], 3), TOKENS // TOK_DEV)
    routes = jax.vmap(lambda own, number: routed_block(jax.random.fold_in(keys[1], 2), own, number, TOK_DEV, EXPERTS, TOP_K, CAP, 0))(routes_keys, routes_turns).reshape((TOKENS, TOP_K))
    route_weight = jnp.clip(0.1 + 0.9 * jax.random.uniform(keys[2], (TOKENS, TOP_K), jnp.float32) ** steps_of(keys[2], (TOKENS, TOP_K), ((0, 8),), -0.2, 0.2), 0.1, 1.0)
    norm_gain = jnp.clip(1.0 + 0.18 * jax.random.normal(keys[3], (D,), jnp.float32), 0.1, 1.9)
    expert_gate = noise(keys[4], (EXPERTS, D, FF), D ** -0.5, 0.125, ((1, 8), (2, 4)), jnp.float32)
    expert_up = noise(keys[5], (EXPERTS, D, FF), D ** -0.5, 0.125, ((1, 8), (2, 4)), jnp.float32)
    expert_down = noise(keys[6], (EXPERTS, D, FF), FF ** -0.5, 0.25, ((1, 8), (2, 4)), jnp.float32)
    shared_gate = noise(keys[7], (D, FF), D ** -0.5, 0.125, ((0, 8), (1, 4)), jnp.float32)
    shared_up = noise(keys[8], (D, FF), D ** -0.5, 0.125, ((0, 8), (1, 4)), jnp.float32)
    shared_down = noise(keys[9], (FF, D), FF ** -0.5, 0.25, ((0, 4), (1, 8)), jnp.float32)
    return {"tokens": tokens, "routes": routes, "route_weight": route_weight, "norm_gain": norm_gain, "expert_gate": expert_gate, "expert_up": expert_up, "expert_down": expert_down, "shared_gate": shared_gate, "shared_up": shared_up, "shared_down": shared_down}


EPS = 1e-06

def slot_places(routes):
    blocks = routes.reshape(N_FS, TOK_DEV * TOP_K)
    onehot = (blocks[:, :, None] == jnp.arange(EXPERTS, dtype=jnp.int32)[None, None, :]).astype(jnp.int32)
    earlier = jnp.cumsum(onehot, axis=1) - onehot
    position = lax.optimization_barrier(jnp.sum(earlier * onehot, axis=2))
    return (blocks * CAP + position).astype(jnp.int32)

def to_sampler(folded):
    return folded.reshape(EXPERTS, D, N_TP, 2, UNITS).transpose(0, 3, 1, 2, 4).reshape(2 * EXPERTS, D, N_TP * UNITS)

def reference(tokens, routes, route_weight, norm_gain, expert_gate, expert_up, expert_down, shared_gate, shared_up, shared_down):
    gate_folded = (expert_gate * norm_gain[None, :, None]).astype(jnp.bfloat16)
    up_folded = (expert_up * norm_gain[None, :, None]).astype(jnp.bfloat16)
    down_round = expert_down.astype(jnp.bfloat16)
    gate_sampler = to_sampler(gate_folded)
    up_sampler = to_sampler(up_folded)
    down_sampler = to_sampler(down_round)
    shared_gate_out = (shared_gate * norm_gain[:, None]).astype(jnp.bfloat16)
    shared_up_out = (shared_up * norm_gain[:, None]).astype(jnp.bfloat16)
    shared_down_out = shared_down.astype(jnp.bfloat16)
    tokens_wide = tokens.astype(jnp.float32)
    normed = (tokens_wide * lax.rsqrt(lax.optimization_barrier(jnp.mean(tokens_wide * tokens_wide, axis=1, keepdims=True)) + EPS)).astype(jnp.bfloat16)
    shared_act = jnp.dot(normed, shared_gate_out, preferred_element_type=jnp.float32)
    shared_lin = jnp.dot(normed, shared_up_out, preferred_element_type=jnp.float32)
    shared_hidden = (jax.nn.silu(shared_act) * shared_lin).astype(jnp.bfloat16)
    shared_sum = jnp.zeros((TOKENS, D), jnp.float32)
    for tp_part in range(N_TP):
        lower = tp_part * SHARED_BLOCK
        product = jnp.dot(shared_hidden[:, lower:lower + SHARED_BLOCK], shared_down_out[lower:lower + SHARED_BLOCK], preferred_element_type=jnp.float32)
        shared_sum = shared_sum + lax.optimization_barrier(product.astype(jnp.bfloat16)).astype(jnp.float32)
    places = slot_places(routes)
    block_ids = jnp.arange(N_FS, dtype=jnp.int32)[:, None]
    token_ids = (block_ids * TOK_DEV + jnp.arange(TOK_DEV * TOP_K, dtype=jnp.int32)[None, :] // TOP_K).astype(jnp.int32)
    slot_table = jnp.full((N_FS, EXPERTS * CAP), TOKENS, jnp.int32).at[block_ids, places].set(token_ids)
    slot_weight = jnp.zeros((N_FS, EXPERTS * CAP), jnp.float32).at[block_ids, places].set(route_weight.reshape(N_FS, TOK_DEV * TOP_K))
    slot_table = slot_table.reshape(N_FS, EXPERTS, CAP).transpose(1, 0, 2).reshape(EXPERTS, N_FS * CAP)
    slot_weight = slot_weight.reshape(N_FS, EXPERTS, CAP).transpose(1, 0, 2).reshape(EXPERTS, N_FS * CAP)
    padded = jnp.concatenate([normed, jnp.zeros((1, D), jnp.bfloat16)], axis=0)

    def expert_step(totals, inputs):
        row_ids, weights, gate_rows, up_rows, down_rows = inputs
        picked = padded[row_ids]
        gate_act = jnp.dot(picked, gate_rows, preferred_element_type=jnp.float32)
        up_act = jnp.dot(picked, up_rows, preferred_element_type=jnp.float32)
        hidden = (jax.nn.silu(gate_act) * up_act).astype(jnp.bfloat16).reshape(N_FS * CAP, N_TP, 2, UNITS)
        down_parts = down_rows.reshape(D, N_TP, 2, UNITS)
        combined = jnp.zeros((N_FS * CAP, D), jnp.float32)
        for half_index in range(2):
            down_half = down_parts[:, :, half_index, :].reshape(D, N_TP * UNITS)
            product = jnp.dot(hidden[:, :, half_index, :].reshape(N_FS * CAP, N_TP * UNITS), down_half.T, preferred_element_type=jnp.float32)
            combined = combined + lax.optimization_barrier(product.astype(jnp.bfloat16)).astype(jnp.float32)
        return (totals.at[row_ids].add(combined * weights[:, None]), None)
    routed_total, _ = lax.scan(expert_step, jnp.zeros((TOKENS + 1, D), jnp.float32), (slot_table, slot_weight, gate_folded, up_folded, down_round))
    mixed = (shared_sum + routed_total[:TOKENS]).astype(jnp.bfloat16)
    return (mixed, gate_sampler, up_sampler, down_sampler, shared_gate_out, shared_up_out, shared_down_out)
```

```python
import jax
import jax.numpy as jnp
from jax import lax
from jax.sharding import PartitionSpec as P

EPS = 1e-06


def swap(value, axis, bit):
    size = lax.axis_size(axis)
    return lax.ppermute(value, axis, [(source, source ^ bit) for source in range(size)])


def bits_of(count):
    return [1 << place for place in reversed(range(count.bit_length() - 1))]


def in_order(own, other, upper, dim):
    return jnp.where(
        upper, jnp.stack([other, own], axis=dim), jnp.stack([own, other], axis=dim)
    )


def doubled(value, axis):
    index = lax.axis_index(axis)
    for step, bit in enumerate(bits_of(lax.axis_size(axis))):
        value = in_order(value, swap(value, axis, bit), (index & bit) != 0, step)
    return value.reshape((lax.axis_size(axis),) + value.shape[len(bits_of(lax.axis_size(axis))):])


def parts_of(value, axis):
    masks, parts = [0], value[None]
    for bit in bits_of(lax.axis_size(axis)):
        parts = jnp.concatenate([parts, swap(parts, axis, bit)], axis=0)
        masks = masks + [mask ^ bit for mask in masks]
    return masks, parts


def product_of_parts(masks, parts, blocks, index, dims):
    total = None
    for place, mask in enumerate(masks):
        block = lax.dynamic_index_in_dim(blocks, index ^ mask, 0, keepdims=False)
        term = lax.dot_general(parts[place], block, (dims, ((), ())), preferred_element_type=jnp.float32)
        total = term if total is None else total + term
    return total


def hidden_of(masks, parts, blocks, index, model_width):
    both = product_of_parts(masks, parts, blocks, index, ((1,), (0,)))
    wide = parts.astype(jnp.float32)
    scale = lax.rsqrt(jnp.sum(wide * wide, axis=(0, 2)) / model_width + EPS)
    gate, up = jnp.split(both * scale[:, None], 2, axis=1)
    return (jax.nn.silu(gate) * up).astype(jnp.bfloat16)


def on_device(
    tokens,
    routes,
    route_weight,
    norm_gain,
    expert_gate,
    expert_up,
    expert_down,
    shared_gate,
    shared_up,
    shared_down,
):
    fs_count = lax.axis_size("fs")
    tp_count = lax.axis_size("tp")
    expert_count, row_share, col_share = expert_gate.shape
    unit_count = col_share // 2
    model_width = row_share * fs_count
    quarter = model_width // tp_count
    tok_count, pick_count = routes.shape
    capacity = 2 * ((3 * tok_count * pick_count + 4 * expert_count - 1) // (4 * expert_count))
    slot_count = expert_count * capacity
    fs_index = lax.axis_index("fs")
    tp_index = lax.axis_index("tp")
    half = fs_index % 2
    groups = [[2 * expert + part for expert in range(expert_count)] for part in range(2)]

    def to_experts(value):
        return lax.all_to_all(
            value, "fs", split_axis=0, concat_axis=0, axis_index_groups=groups, tiled=True
        )

    experts = jnp.arange(expert_count, dtype=jnp.int32)
    named = (routes[:, :, None] == experts[None, None, :]).astype(jnp.float32)
    member = jnp.sum(named, axis=1).astype(jnp.bfloat16)
    rows = jnp.arange(tok_count, dtype=jnp.int32)
    before = (rows[:, None] > rows[None, :]).astype(jnp.bfloat16)
    earlier = jnp.dot(before, member, preferred_element_type=jnp.float32)
    position = jnp.sum(named * earlier[:, None, :], axis=2).astype(jnp.int32)
    slot_index = routes * capacity + position
    slots = jnp.arange(slot_count, dtype=jnp.int32)
    picked = (slot_index.T[:, :, None] == slots[None, None, :]).astype(jnp.bfloat16)
    sent = jnp.sum(
        (slot_index.T[:, None, :] == slots[None, :, None]).astype(jnp.float32), axis=0
    ).astype(jnp.bfloat16)
    outgoing = jnp.dot(sent, tokens, preferred_element_type=jnp.float32).astype(jnp.bfloat16)
    arrived = to_experts(outgoing)

    row_gain = norm_gain[None, :, None]
    pair_own = to_experts(
        jnp.concatenate([expert_gate * row_gain, expert_up * row_gain], axis=2).astype(jnp.bfloat16)
    )
    down_own = to_experts(expert_down.astype(jnp.bfloat16))
    pair_full = in_order(pair_own, swap(pair_own, "fs", 1), half == 1, 1).reshape(
        model_width, 2 * col_share
    )
    down_cols = lax.all_to_all(
        down_own.reshape(tp_count, expert_count // tp_count, row_share, col_share),
        "tp",
        split_axis=0,
        concat_axis=0,
        tiled=True,
    )
    down_full = in_order(down_cols, swap(down_cols, "fs", 1), half == 1, 2).reshape(
        tp_count, quarter, col_share
    )
    halves = lax.dynamic_index_in_dim(
        pair_full.reshape(model_width, 2, 2, unit_count), half, 2, keepdims=False
    )
    gate_new = halves[None, :, 0]
    up_new = halves[None, :, 1]
    down_new = (
        lax.dynamic_index_in_dim(
            down_full.reshape(tp_count, quarter, 2, unit_count), half, 2, keepdims=False
        )
        .transpose(1, 0, 2)
        .reshape(1, quarter, tp_count * unit_count)
    )

    shared_pair = jnp.concatenate(
        [shared_gate * norm_gain[:, None], shared_up * norm_gain[:, None]], axis=1
    ).astype(jnp.bfloat16)
    packed_down = shared_down.astype(jnp.bfloat16).reshape(row_share // 2, 2 * col_share)
    packed = jnp.concatenate([shared_pair, packed_down], axis=0)
    shared_all = doubled(packed, "fs")
    shared_pair_new = shared_all[:, :row_share].reshape(model_width, 2 * col_share)
    shared_gate_new = shared_pair_new[:, :col_share]
    shared_up_new = shared_pair_new[:, col_share:]
    shared_down_new = (
        shared_all[:, row_share:]
        .reshape(fs_count, col_share, row_share)
        .transpose(1, 0, 2)
        .reshape(col_share, model_width)
    )
    masks, own_parts = parts_of(tokens, "tp")
    shared_hidden = hidden_of(
        masks,
        own_parts,
        shared_pair_new.reshape(tp_count, quarter, 2 * col_share),
        tp_index,
        model_width,
    )
    shared_term = jnp.dot(
        shared_hidden, shared_down_new, preferred_element_type=jnp.float32
    ).astype(jnp.bfloat16)
    shared_parts = lax.all_to_all(
        shared_term.reshape(tok_count, tp_count, quarter).transpose(1, 0, 2),
        "tp",
        split_axis=0,
        concat_axis=0,
        tiled=True,
    )
    shared_sum = jnp.sum(shared_parts.astype(jnp.float32), axis=0)

    masks, arrived_parts = parts_of(arrived, "tp")
    hidden = hidden_of(
        masks,
        arrived_parts,
        pair_full.reshape(tp_count, quarter, 2 * col_share),
        tp_index,
        model_width,
    )
    masks, hidden_parts = parts_of(hidden, "tp")
    expert_sum = product_of_parts(
        masks, hidden_parts, down_full, tp_index, ((1,), (1,))
    ).astype(jnp.bfloat16)
    returned = to_experts(expert_sum)
    chosen = jnp.dot(
        picked.reshape(pick_count * tok_count, slot_count),
        returned,
        preferred_element_type=jnp.float32,
    ).reshape(pick_count, tok_count, quarter)
    routed = jnp.sum(chosen * route_weight.T[:, :, None], axis=0)
    mixed = (shared_sum + routed).astype(jnp.bfloat16)
    return (mixed, gate_new, up_new, down_new, shared_gate_new, shared_up_new, shared_down_new)


def solution(mesh):
    in_specs = (
        P("fs", "tp"),
        P("fs", None),
        P("fs", None),
        P("fs"),
        P(None, "fs", "tp"),
        P(None, "fs", "tp"),
        P(None, "fs", "tp"),
        P("fs", "tp"),
        P("fs", "tp"),
        P("tp", "fs"),
    )
    out_specs = (
        P("fs", "tp"),
        P("fs", None, "tp"),
        P("fs", None, "tp"),
        P("fs", "tp", None),
        P(None, "tp"),
        P(None, "tp"),
        P("tp", None),
    )
    return jax.shard_map(
        on_device, mesh=mesh, in_specs=in_specs, out_specs=out_specs, check_vma=False
    )
```
